32 devices in a mesh: rep: 2 (over x), fs: 8 (over z, y), tp: 2 (over core).
Axes of the slice: x: 2, y: 2, z: 4, core: 2. Of those that a mesh axis runs over, the one named last changes fastest.
Arguments:
- stream: bfloat16 [4096, 2048], P(('rep', 'fs'), 'tp'), may hold values from -6 to 6
- norm_gains: float32 [6, 2048], replicated, may hold values from 0.1 to 1.9
- w_gate: bfloat16 [2048, 5632], P('fs', 'tp'), may hold values from -0.125 to 0.125
- w_up: bfloat16 [2048, 5632], P('fs', 'tp'), may hold values from -0.125 to 0.125
- w_down: bfloat16 [5632, 2048], P('tp', 'fs'), may hold values from -0.109375 to 0.109375
- w_inner: bfloat16 [2048, 1024], P('fs', 'tp'), may hold values from -0.125 to 0.125
- w_bgate: bfloat16 [2048, 1024], P('fs', 'tp'), may hold values from -0.125 to 0.125
- w_cgate: bfloat16 [2048, 1024], P('fs', 'tp'), may hold values from -0.125 to 0.125
- conv_taps: float32 [3, 1024], P(None, 'tp'), may hold values from -3.5 to 3.5
- w_out: bfloat16 [1024, 2048], P('tp', 'fs'), may hold values from -0.25 to 0.25
Outputs:
- mixed: bfloat16 [4096, 2048], P(('rep', 'fs'), 'tp')
The draws below stay inside these ranges and needn't reach their ends.
All inputs are finite; a program needn't handle non-finite values.
Results may differ from the reference program's by a relative error of at most 0.02.
Values may be sent and summed in bfloat16 or wider, within the bound.
No kernel may reach another device: no remote copies, remote signals or barrier semaphores. Data moves between devices by JAX's collectives and lax.ppermute only.
A program may use at most 128 MiB of HBM per device.

```python
import jax
import jax.numpy as jnp
from jax import lax

D = 2048
FF = 5632
CW = 1024
TAPS = 3
SEQ_LEN = 2048
TOKENS = 4096
N_TP = 2


def strengthened(values, rng, source, target, shards_of, factor):
    def block_of(position):
        return (jnp.arange(values.shape[position]) // (values.shape[position] // shards_of)).reshape((-1,) + (1,) * (values.ndim - 1 - position))

    one_side = jax.random.permutation(rng, shards_of)[block_of(target)]
    second = (block_of(target) + shards_of // 2) % shards_of
    return jnp.where((block_of(source) == one_side) | (block_of(source) == second), factor * values, values)


def levels(key, extent, pieces, least, largest):
    level, own = 1.0, jax.random.fold_in(key, 6)
    for dim, blocks in pieces:
        draws = jnp.exp(jax.random.uniform(jax.random.fold_in(own, dim), (blocks,), jnp.float32, least / len(pieces), largest / len(pieces)))
        level = level * jnp.repeat(draws, extent[dim] // blocks).reshape([-1 if axis == dim else 1 for axis in range(len(extent))])
    return level


def normal_values(rng, dims, width, limit, cuts=(), held_as=jnp.bfloat16):
    array = jax.random.normal(rng, dims, jnp.float32) * width
    if len(cuts) > 0:
        array = levels(rng, dims, cuts, -0.22, 0.18) * array
    return jnp.clip(array, min=-limit, max=limit).astype(held_as)


def noise_with(rng, extent, deviation, most, shards, heavy, dtype=jnp.bfloat16):
    values = deviation * jax.random.normal(rng, extent, jnp.float32)
    if shards:
        values = values * levels(rng, extent, shards, -0.22, 0.18)
    return jnp.clip(strengthened(values, jax.random.fold_in(rng, 3), *heavy), -most, most).astype(dtype)


def setup_inputs(seed: int = 0) -> dict:
    key_list = jax.random.split(jax.random.key(seed), 11)
    return {
        "stream": normal_values(key_list[0], (TOKENS, D), 1.0, 6.0, ((0, 16), (1, 2))),
        "norm_gains": jnp.clip(1.0 + 0.18 * jax.random.normal(key_list[1], (6, D), jnp.float32), 0.1, 1.9),
        "w_gate": normal_values(key_list[2], (D, FF), D ** -0.5, 0.125, ((0, 8), (1, 2))),
        "w_up": normal_values(key_list[3], (D, FF), D ** -0.5, 0.125, ((0, 8), (1, 2))),
        "w_down": noise_with(key_list[4], (FF, D), FF ** -0.5, 0.109375, ((0, 2), (1, 8)), (0, 1, 8, 2.0)),
        "w_inner": normal_values(key_list[5], (D, CW), D ** -0.5, 0.125, ((0, 8), (1, 2))),
        "w_bgate": normal_values(key_list[6], (D, CW), D ** -0.5, 0.125, ((0, 8), (1, 2))),
        "w_cgate": normal_values(key_list[7], (D, CW), D ** -0.5, 0.125, ((0, 8), (1, 2))),
        "conv_taps": normal_values(key_list[8], (TAPS, CW), TAPS ** -0.5, 3.5, ((1, 2),), jnp.float32),
        "w_out": noise_with(key_list[9], (CW, D), CW ** -0.5, 0.25, ((0, 2), (1, 8)), (0, 1, 8, 2.0)),
    }


EPSILON = 1e-06

def rms_scale(values):
    return values * lax.rsqrt(lax.optimization_barrier(jnp.mean(values * values, axis=1, keepdims=True)) + EPSILON)

def norm_input(current, gain):
    return (rms_scale(current.astype(jnp.float32)) * gain).astype(jnp.bfloat16)

def split_sum(hidden, weight, groups):
    columns = hidden.shape[1] // groups
    result = jnp.zeros((hidden.shape[0], weight.shape[1]), jnp.float32)
    for group in range(groups):
        partial_term = jnp.dot(hidden[:, group * columns:(group + 1) * columns], weight[group * columns:(group + 1) * columns], preferred_element_type=jnp.float32)
        rounded = lax.optimization_barrier(partial_term.astype(jnp.bfloat16))
        result = result + rounded.astype(jnp.float32)
    return result

def settle(current, branch_sum, gain, weight):
    return (current.astype(jnp.float32) + weight * (rms_scale(branch_sum) * gain)).astype(jnp.bfloat16)

def feed_forward(current, gain_in, gain_out, w_gate, w_up, w_down):
    normed = norm_input(current, gain_in)
    gate_vals = jnp.dot(normed, w_gate, preferred_element_type=jnp.float32)
    upward = jnp.dot(normed, w_up, preferred_element_type=jnp.float32)
    hidden = (jax.nn.silu(gate_vals) * upward).astype(jnp.bfloat16)
    return settle(current, split_sum(hidden, w_down, N_TP), gain_out, 0.5)

def reference(stream, norm_gains, w_gate, w_up, w_down, w_inner, w_bgate, w_cgate, conv_taps, w_out):
    first = feed_forward(stream, norm_gains[0], norm_gains[1], w_gate, w_up, w_down)
    normed = norm_input(first, norm_gains[2])
    inner = jnp.dot(normed, w_inner, preferred_element_type=jnp.float32)
    bgate = jnp.dot(normed, w_bgate, preferred_element_type=jnp.float32)
    cgate = jnp.dot(normed, w_cgate, preferred_element_type=jnp.float32)
    conv_input = (cgate * inner).reshape(-1, SEQ_LEN, CW)
    padded = jnp.pad(conv_input, ((0, 0), (TAPS - 1, 0), (0, 0)))
    conv = conv_taps[0] * padded[:, 0:SEQ_LEN]
    for tap in range(1, TAPS):
        conv = conv + conv_taps[tap] * padded[:, tap:tap + SEQ_LEN]
    gated = (bgate * conv.reshape(-1, CW)).astype(jnp.bfloat16)
    second = settle(first, split_sum(gated, w_out, N_TP), norm_gains[3], 1.0)
    return feed_forward(second, norm_gains[4], norm_gains[5], w_gate, w_up, w_down)
```

```python
import functools
import itertools

import jax
import jax.numpy as jnp
from jax import lax
from jax.experimental import pallas as pl
from jax.experimental.pallas import tpu as pltpu
from jax.sharding import Mesh, PartitionSpec as P

TAPS = 3
EPSILON = 1e-06
NT = (((1,), (1,)), ((), ()))
NN = (((1,), (0,)), ((), ()))
DEPTH = ("zh", "zp")


def moved(x, axes, by):
    count = lax.axis_size(axes)
    if by % count == 0:
        return x
    return lax.ppermute(x, axes, [(i, (i + by) % count) for i in range(count)])


def whole(shape):
    return pl.BlockSpec(shape, lambda *_: (0,) * len(shape))


def normed_rows(rows, gain):
    values = rows.astype(jnp.float32)
    scale = lax.rsqrt(jnp.mean(values * values, axis=1, keepdims=True) + EPSILON)
    return (values * scale * gain).astype(jnp.bfloat16)


def join_columns(where, first, parts, target):
    for j, part in enumerate(parts):
        width = part.shape[1]
        if len(parts) == 1:
            target[...] = part[...]
        else:
            target[:, pl.ds(pl.multiple_of(where[first + j] * width, width), width)] = part[...]


def join_rows(where, first, parts, target, columns=None):
    for j, part in enumerate(parts):
        height = part.shape[0]
        target[pl.ds(pl.multiple_of(where[first + j] * height, height), height), :] = part[...]


def up_kernel(blocks, parts, where, gain, *refs):
    gates, ups, rows = refs[:blocks], refs[blocks : 2 * blocks], refs[2 * blocks : 2 * blocks + parts]
    out, gate_all, up_all, row_all = refs[2 * blocks + parts :]

    @pl.when(pl.program_id(0) == 0)
    def _():
        join_columns(where, 0, gates, gate_all)
        join_columns(where, 0, ups, up_all)

    join_columns(where, blocks, rows, row_all)
    normed = normed_rows(row_all[...], gain[...])
    gate_vals = lax.dot_general(normed, gate_all[...], NT, preferred_element_type=jnp.float32)
    upward = lax.dot_general(normed, up_all[...], NT, preferred_element_type=jnp.float32)
    out[...] = (gate_vals / (1.0 + jnp.exp(-gate_vals)) * upward).astype(out.dtype)


def split_columns(where, first, result, outs, scratch):
    scratch[...] = result
    width = outs[0].shape[1]
    for t, out in enumerate(outs):
        out[...] = scratch[:, pl.ds(pl.multiple_of(where[first + t] * width, width), width)].astype(out.dtype)


def down_kernel(blocks, parts, where, hidden, *refs):
    downs, outs = refs[:blocks], refs[blocks : blocks + parts]
    down_all, result = refs[blocks + parts :]

    @pl.when(pl.program_id(0) == 0)
    def _():
        join_columns(where, 0, downs, down_all)

    split_columns(
        where, blocks, lax.dot_general(hidden[...], down_all[...], NN, preferred_element_type=jnp.float32), outs, result
    )


def mix_in_kernel(blocks, parts, where, gain, *refs):
    mats, rows = refs[:blocks], refs[blocks : blocks + parts]
    conv_input, bgate, mat_all, row_all = refs[blocks + parts :]
    join_rows(where, 0, mats, mat_all)
    join_columns(where, blocks, rows, row_all)
    normed = normed_rows(row_all[...], gain[...])
    width = bgate.shape[1]
    values = lax.dot_general(normed, mat_all[...], NN, preferred_element_type=jnp.float32)
    bgate[...] = values[:, width : 2 * width]
    conv_input[...] = values[:, :width] * values[:, 2 * width :]


def mix_out_kernel(blocks, parts, where, conv_input, earlier, bgate, taps, *refs):
    mats, outs = refs[:blocks], refs[blocks : blocks + parts]
    mat_all, padded, result = refs[blocks + parts :]
    rows = conv_input.shape[0]
    join_rows(where, 0, mats, mat_all)
    padded[8 - (TAPS - 1) : 8, :] = earlier[...]
    padded[8:, :] = conv_input[...]
    conv = taps[0:1, :] * padded[8 - (TAPS - 1) : 8 - (TAPS - 1) + rows, :]
    for tap in range(1, TAPS):
        start = 8 - (TAPS - 1) + tap
        conv = conv + taps[tap : tap + 1, :] * padded[start : start + rows, :]
    gated = (bgate[...] * conv).astype(jnp.bfloat16)
    split_columns(
        where, blocks, lax.dot_general(gated, mat_all[...], NT, preferred_element_type=jnp.float32), outs, result
    )


def shards(stream, norm_gains, w_gate, w_up, w_down, w_inner, w_bgate, w_cgate, conv_taps, w_out):
    reps, deep, wide, cores = (lax.axis_size(a) for a in ("rep", DEPTH, "y", "tp"))
    pair = lax.axis_size("zp")
    rep, z, zp, y, core = (lax.axis_index(a) for a in ("rep", DEPTH, "zp", "y", "tp"))
    tokens, local_width = stream.shape
    model_width = local_width * cores
    block_width = w_gate.shape[0]
    group = reps * pair
    hidden_width = w_gate.shape[1] // group
    channels = w_inner.shape[1]
    params = pltpu.CompilerParams(vmem_limit_bytes=56 * 2**20)

    core_order = jnp.stack([(core - t) % cores for t in range(cores)]).astype(jnp.int32)
    core_targets = jnp.stack([(core + t) % cores for t in range(cores)]).astype(jnp.int32)
    offsets = list(itertools.product(range(deep), range(wide)))
    block_order = jnp.stack([(z - d) % deep * wide + (y - e) % wide for d, e in offsets]).astype(jnp.int32)

    def pieces(matrix):
        return lax.dynamic_index_in_dim(matrix.reshape(reps, pair, hidden_width, block_width), rep, 0, False)

    def gathered(matrix):
        by_pair = pieces(matrix)
        found = []
        for d in range(deep):
            piece = moved(lax.dynamic_index_in_dim(by_pair, (zp + d) % pair, 0, False), DEPTH, d)
            found += [moved(piece, "y", e) for e in range(wide)]
        return found

    gates, ups, downs = gathered(w_gate.T), gathered(w_up.T), gathered(w_down)
    ff_order = block_order
    if block_width % 128:

        def joined(blocks):
            target = jnp.zeros((hidden_width, model_width), jnp.bfloat16)
            for j, block in enumerate(blocks):
                target = lax.dynamic_update_slice(target, block, (0, block_order[j] * block_width))
            return [target]

        gates, ups, downs = joined(gates), joined(ups), joined(downs)
        ff_order = jnp.zeros((1,), jnp.int32)
    ff_blocks = len(gates)
    ff_block_width = gates[0].shape[1]

    mixer = jnp.concatenate([w_inner, w_bgate, w_cgate, w_out.T], axis=1)
    share = block_width // reps
    own = lax.dynamic_slice_in_dim(mixer, rep * share, share, 0)
    ahead, behind, right, left = [own], [own], own, own
    for step in range(1, deep):
        right = lax.ppermute(right, DEPTH, [(i, i + 1) for i in range(step - 1, deep - 1)])
        left = lax.ppermute(left, DEPTH, [(i, i - 1) for i in range(1, deep - step + 1)])
        behind.append(right)
        ahead.append(left)
    mats, mat_order = [], []
    for d in range(deep):
        piece = own if d == 0 else jnp.where(z >= d, behind[d], ahead[deep - d])
        for e in range(wide):
            beside = moved(piece, "y", e)
            for h in range(reps):
                mats.append(moved(beside, "rep", h))
                mat_order.append(((z - d) % deep * wide + (y - e) % wide) * reps + (rep - h) % reps)
    mat_order = jnp.stack(mat_order).astype(jnp.int32)

    def across_cores(rows):
        return [moved(rows, "tp", t) for t in range(cores)]

    members = list(itertools.product(range(reps), range(pair)))

    def to_member(x, dr, dp):
        if dr == 0 and dp == 0:
            return x
        places = list(itertools.product(range(reps), range(pair)))
        return lax.ppermute(
            x,
            ("rep", "zp"),
            [(r * pair + p, (r + dr) % reps * pair + (p + dp) % pair) for r, p in places],
        )

    def settle(current, branch, row, weight):
        squares = jnp.sum(branch * branch, axis=1, keepdims=True)
        squares = sum(across_cores(squares))
        gain = lax.dynamic_slice_in_dim(norm_gains[row], core * local_width, local_width, 0)
        scaled = branch * lax.rsqrt(squares / model_width + EPSILON)
        return (current.astype(jnp.float32) + weight * (scaled * gain)).astype(jnp.bfloat16)

    def core_sum(shares):
        total = shares[0].astype(jnp.float32)
        for t in range(1, cores):
            total = total + moved(shares[t], "tp", t).astype(jnp.float32)
        return total

    def feed_forward(current, row_in, row_out):
        stacked = jnp.concatenate([to_member(current, dr, dp) for dr, dp in members], axis=0)
        parts = across_cores(stacked)
        count = group * tokens
        hidden = pl.pallas_call(
            functools.partial(up_kernel, ff_blocks, cores),
            grid_spec=pltpu.PrefetchScalarGridSpec(
                num_scalar_prefetch=1,
                grid=(group,),
                in_specs=[whole((1, model_width))]
                + [whole((hidden_width, ff_block_width))] * (2 * ff_blocks)
                + [pl.BlockSpec((tokens, local_width), lambda i, *_: (i, 0))] * cores,
                out_specs=pl.BlockSpec((tokens, hidden_width), lambda i, *_: (i, 0)),
                scratch_shapes=[
                    pltpu.VMEM((hidden_width, model_width), jnp.bfloat16),
                    pltpu.VMEM((hidden_width, model_width), jnp.bfloat16),
                    pltpu.VMEM((tokens, model_width), jnp.bfloat16),
                ],
            ),
            out_shape=jax.ShapeDtypeStruct((count, hidden_width), jnp.bfloat16),
            compiler_params=params,
            name="up",
        )(jnp.concatenate([ff_order, core_order]), norm_gains[row_in : row_in + 1], *gates, *ups, *parts)
        shares = pl.pallas_call(
            functools.partial(down_kernel, ff_blocks, cores),
            grid_spec=pltpu.PrefetchScalarGridSpec(
                num_scalar_prefetch=1,
                grid=(group,),
                in_specs=[pl.BlockSpec((tokens, hidden_width), lambda i, *_: (i, 0))]
                + [whole((hidden_width, ff_block_width))] * ff_blocks,
                out_specs=[pl.BlockSpec((tokens, local_width), lambda i, *_: (i, 0))] * cores,
                scratch_shapes=[
                    pltpu.VMEM((hidden_width, model_width), jnp.bfloat16),
                    pltpu.VMEM((tokens, model_width), jnp.float32),
                ],
            ),
            out_shape=[jax.ShapeDtypeStruct((count, local_width), jnp.bfloat16)] * cores,
            compiler_params=params,
            name="down",
        )(jnp.concatenate([ff_order, core_targets]), hidden, *downs)
        sums = core_sum(shares)
        branch = sums[:tokens]
        for m, (dr, dp) in enumerate(members):
            if m:
                given = sums[m * tokens : (m + 1) * tokens].astype(jnp.bfloat16)
                branch = branch + to_member(given, -dr, -dp).astype(jnp.float32)
        return settle(current, branch, row_out, 0.5)

    def mix(current):
        parts = across_cores(current)
        blocks = len(mats)
        conv_input, bgate = pl.pallas_call(
            functools.partial(mix_in_kernel, blocks, cores),
            grid_spec=pltpu.PrefetchScalarGridSpec(
                num_scalar_prefetch=1,
                grid=(1,),
                in_specs=[whole((1, model_width))]
                + [whole((share, 3 * channels))] * blocks
                + [whole((tokens, local_width))] * cores,
                out_specs=[whole((tokens, channels))] * 2,
                scratch_shapes=[
                    pltpu.VMEM((model_width, 3 * channels), jnp.bfloat16),
                    pltpu.VMEM((tokens, model_width), jnp.bfloat16),
                ],
            ),
            out_shape=[jax.ShapeDtypeStruct((tokens, channels), jnp.float32)] * 2,
            compiler_params=params,
            name="mix_in",
        )(jnp.concatenate([mat_order, core_order]), norm_gains[2:3], *mats, *parts)
        count = deep * wide
        earlier = lax.ppermute(
            conv_input[tokens - (TAPS - 1) :], DEPTH + ("y",), [(i, i + 1) for i in range(count - 1)]
        )
        shares = pl.pallas_call(
            functools.partial(mix_out_kernel, blocks, cores),
            grid_spec=pltpu.PrefetchScalarGridSpec(
                num_scalar_prefetch=1,
                grid=(1,),
                in_specs=[
                    whole((tokens, channels)),
                    whole((TAPS - 1, channels)),
                    whole((tokens, channels)),
                    whole((TAPS, channels)),
                ]
                + [pl.BlockSpec((share, channels), lambda *_: (0, 3))] * blocks,
                out_specs=[whole((tokens, local_width))] * cores,
                scratch_shapes=[
                    pltpu.VMEM((model_width, channels), jnp.bfloat16),
                    pltpu.VMEM((tokens + 8, channels), jnp.float32),
                    pltpu.VMEM((tokens, model_width), jnp.float32),
                ],
            ),
            out_shape=[jax.ShapeDtypeStruct((tokens, local_width), jnp.bfloat16)] * cores,
            compiler_params=params,
            name="mix_out",
        )(jnp.concatenate([mat_order, core_targets]), conv_input, earlier, bgate, conv_taps, *mats)
        return settle(current, core_sum(shares), 3, 1.0)

    first = feed_forward(stream, 0, 1)
    second = mix(first)
    return feed_forward(second, 4, 5)


def solution(mesh):
    reps, count, cores = (mesh.shape[a] for a in ("rep", "fs", "tp"))
    wide = 1
    while 8 * wide * wide <= count and count % (2 * wide) == 0:
        wide *= 2
    deep = count // wide
    pair = 2 if deep % 2 == 0 else 1
    fine = Mesh(mesh.devices.reshape(reps, deep // pair, pair, wide, cores), ("rep", "zh", "zp", "y", "tp"))
    position = ("zh", "zp", "y")
    return jax.shard_map(
        shards,
        mesh=fine,
        in_specs=(
            P(("rep",) + position, "tp"),
            P(),
            P(position, "tp"),
            P(position, "tp"),
            P("tp", position),
            P(position, "tp"),
            P(position, "tp"),
            P(position, "tp"),
            P(None, "tp"),
            P("tp", position),
        ),
        out_specs=P(("rep",) + position, "tp"),
        check_vma=False,
    )
```
